32 devices in a mesh: sp: 4 (over y, x), tp: 8 (over z, core).
Axes of the slice: x: 2, y: 2, z: 4, core: 2. Of those that a mesh axis runs over, the one named last changes fastest.
Arguments:
- target: bfloat16 [512, 2048], P('sp'), may hold values from -6 to 6
- source: bfloat16 [1536, 2048], P('sp'), may hold values from -6 to 6
- cotangent: bfloat16 [512, 2048], P('sp'), may hold values from -192 to 192
- target_gain: float32 [2048], replicated, may hold values from 0.1 to 1.9
- source_gain: float32 [2048], replicated, may hold values from 0.1 to 1.9
- w_query: bfloat16 [2048, 4096], P(None, 'tp'), may hold values from -0.125 to 0.125
- w_key: bfloat16 [2048, 128], replicated, may hold values from -0.125 to 0.125
- w_value: bfloat16 [2048, 128], replicated, may hold values from -0.125 to 0.125
- w_out: bfloat16 [4096, 2048], P('tp'), may hold values from -0.09375 to 0.09375
Outputs:
- grad_target: bfloat16 [512, 2048], P(('sp', 'tp'))
- grad_source: bfloat16 [1536, 2048], P(('sp', 'tp'))
- grad_out_w: bfloat16 [4096, 2048], P('tp', 'sp')
The draws below stay inside these ranges and needn't reach their ends.
All inputs are finite; a program needn't handle non-finite values.
Results may differ from the reference program's by a relative error of at most 0.025.
Values may be sent and summed in bfloat16 or wider, within the bound.
No kernel may reach another device: no remote copies, remote signals or barrier semaphores. Data moves between devices by JAX's collectives and lax.ppermute only.
A program may use at most 64 MiB of HBM per device.

```python
import jax
import jax.numpy as jnp
from jax import lax

D = 2048
HEADS = 32
HEAD = 128
TARGET = 512
SOURCE = 1536


def steps_of(own_key, dims, shards, low, largest):
    level = 1.0
    for dim, shards_of in shards:
        draws = jax.random.uniform(jax.random.fold_in(jax.random.fold_in(own_key, 6), dim), (shards_of,), jnp.float32, low / len(shards), largest / len(shards))
        level = level * jnp.repeat(jnp.exp(draws), dims[dim] // shards_of).reshape((-1,) + (1,) * (len(dims) - 1 - dim))
    return level


def bell_draw(own_key, extent, spread, bound, split=(), kind=jnp.bfloat16):
    result = spread * jax.random.normal(own_key, extent, jnp.float32)
    if split:
        result = result * steps_of(own_key, extent, split, -0.22, 0.18)
    return jnp.clip(result, -bound, bound).astype(kind)


def setup_inputs(seed: int = 0) -> dict:
    key_of = jax.random.split(jax.random.key(seed), 10)
    return {
        "target": bell_draw(key_of[0], (TARGET, D), 1.0, 6.0, ((0, 4),)),
        "source": bell_draw(key_of[1], (SOURCE, D), 1.0, 6.0, ((0, 4),)),
        "cotangent": bell_draw(key_of[2], (TARGET, D), 32.0, 192.0, ((0, 4),)),
        "target_gain": jnp.clip(1.0 + 0.18 * jax.random.normal(key_of[3], (D,), jnp.float32), 0.1, 1.9),
        "source_gain": jnp.clip(1.0 + 0.18 * jax.random.normal(key_of[4], (D,), jnp.float32), 0.1, 1.9),
        "w_query": bell_draw(key_of[5], (D, HEADS * HEAD), D ** -0.5, 0.125, ((1, 8),)),
        "w_key": bell_draw(key_of[6], (D, HEAD), D ** -0.5, 0.125),
        "w_value": bell_draw(key_of[7], (D, HEAD), D ** -0.5, 0.125),
        "w_out": bell_draw(key_of[8], (HEADS * HEAD, D), (HEADS * HEAD) ** -0.5, 0.09375, ((0, 8),)),
    }


NORM_EPS = 1e-06

def normed(row_block, gain_vec):
    rows_wide = row_block.astype(jnp.float32)
    inv_rms = lax.rsqrt(lax.optimization_barrier(jnp.mean(rows_wide * rows_wide, axis=1, keepdims=True)) + NORM_EPS)
    return (rows_wide * inv_rms * gain_vec).astype(jnp.bfloat16)

def norm_back(row_block, gain_vec, upstream):
    rows_wide = row_block.astype(jnp.float32)
    inv_rms = lax.rsqrt(lax.optimization_barrier(jnp.mean(rows_wide * rows_wide, axis=1, keepdims=True)) + NORM_EPS)
    unit_rows = rows_wide * inv_rms
    pulled = upstream * gain_vec
    return inv_rms * (pulled - unit_rows * lax.optimization_barrier(jnp.mean(pulled * unit_rows, axis=1, keepdims=True)))

def reference(target, source, cotangent, target_gain, source_gain, w_query, w_key, w_value, w_out):
    inv_root = HEAD ** (-0.5)
    normed_target = normed(target, target_gain)
    query_rows = jnp.dot(normed_target, w_query, preferred_element_type=jnp.float32).astype(jnp.bfloat16)
    normed_source = normed(source, source_gain)
    key_rows = jnp.dot(normed_source, w_key, preferred_element_type=jnp.float32).astype(jnp.bfloat16)
    value_rows = jnp.dot(normed_source, w_value, preferred_element_type=jnp.float32).astype(jnp.bfloat16)
    grad_attn = jnp.dot(cotangent, w_out.T, preferred_element_type=jnp.float32).astype(jnp.bfloat16)
    query_heads = query_rows.reshape(TARGET, HEADS, HEAD).transpose(1, 0, 2)
    grad_heads = grad_attn.reshape(TARGET, HEADS, HEAD).transpose(1, 0, 2)

    def one_head(carried, head_pair):
        key_sum, value_sum = carried
        query_one, grad_one = head_pair
        scores = jnp.dot(query_one, key_rows.T, preferred_element_type=jnp.float32) * inv_root
        exponent = jnp.exp(scores)
        row_total = lax.optimization_barrier(jnp.sum(exponent, axis=1))
        weights = exponent.astype(jnp.bfloat16)
        attended = (jnp.dot(weights, value_rows, preferred_element_type=jnp.float32) / row_total[:, None]).astype(jnp.bfloat16)
        prob_grad = jnp.dot(grad_one, value_rows.T, preferred_element_type=jnp.float32)
        delta_row = lax.optimization_barrier(jnp.sum(attended.astype(jnp.float32) * grad_one.astype(jnp.float32), axis=1))
        tilted = (exponent * prob_grad).astype(jnp.bfloat16)
        tilted_sum = jnp.dot(tilted, key_rows, preferred_element_type=jnp.float32)
        weight_sum = jnp.dot(weights, key_rows, preferred_element_type=jnp.float32)
        grad_query = ((tilted_sum - delta_row[:, None] * weight_sum) / row_total[:, None] * inv_root).astype(jnp.bfloat16)
        prob_rows = exponent / row_total[:, None]
        score_grad = (prob_rows * (prob_grad - delta_row[:, None])).astype(jnp.bfloat16)
        key_grad = jnp.dot(score_grad.T, query_one, preferred_element_type=jnp.float32) * inv_root
        value_grad = jnp.dot(prob_rows.astype(jnp.bfloat16).T, grad_one, preferred_element_type=jnp.float32)
        return ((key_sum + key_grad, value_sum + value_grad), (attended, grad_query))
    empty_keys = jnp.zeros((SOURCE, HEAD), jnp.float32)
    sums, stacked = lax.scan(one_head, (empty_keys, empty_keys), (query_heads, grad_heads))
    key_grad, value_grad = sums
    attended_heads, query_grad_heads = stacked
    attended_rows = attended_heads.transpose(1, 0, 2).reshape(TARGET, HEADS * HEAD)
    query_grad_rows = query_grad_heads.transpose(1, 0, 2).reshape(TARGET, HEADS * HEAD)
    pulled_source = jnp.dot(key_grad.astype(jnp.bfloat16), w_key.T, preferred_element_type=jnp.float32)
    pulled_source = pulled_source + jnp.dot(value_grad.astype(jnp.bfloat16), w_value.T, preferred_element_type=jnp.float32)
    grad_source = norm_back(source, source_gain, pulled_source).astype(jnp.bfloat16)
    pulled_target = jnp.dot(query_grad_rows, w_query.T, preferred_element_type=jnp.float32)
    grad_target = norm_back(target, target_gain, pulled_target).astype(jnp.bfloat16)
    grad_out_w = jnp.dot(attended_rows.T, cotangent, preferred_element_type=jnp.float32).astype(jnp.bfloat16)
    return (grad_target, grad_source, grad_out_w)
```

```python
import functools

import jax
import jax.numpy as jnp
from jax import lax
from jax.experimental import pallas as pl
from jax.experimental.pallas import tpu as pltpu
from jax.sharding import PartitionSpec as P

HEAD = 128
NORM_EPS = 1e-06
LOG2_E = 1.4426950408889634
ROW_TILE = 16
CHUNK = 192

BF16 = jnp.bfloat16
F32 = jnp.float32


VMEM = pl.BlockSpec(memory_space=pltpu.VMEM)
ANY = pl.BlockSpec(memory_space=pl.ANY)


def nn(left, right):
    return lax.dot_general(left, right, (((1,), (0,)), ((), ())), preferred_element_type=F32)


def nt(left, right):
    return lax.dot_general(left, right, (((1,), (1,)), ((), ())), preferred_element_type=F32)


def inverse_rms(rows_wide):
    return lax.rsqrt(jnp.mean(rows_wide * rows_wide, axis=1, keepdims=True) + NORM_EPS)


def normed(rows, gain):
    wide = rows.astype(F32)
    return (wide * inverse_rms(wide) * gain).astype(BF16)


def norm_back(rows, gain, upstream):
    wide = rows.astype(F32)
    inv = inverse_rms(wide)
    unit = wide * inv
    pulled = upstream * gain
    return inv * (pulled - unit * jnp.mean(pulled * unit, axis=1, keepdims=True))


def shape(dims, kind):
    return jax.ShapeDtypeStruct(dims, kind)


def call(body, outs, flops, moved, in_specs, scratch=(), name=None):
    return pl.pallas_call(
        body,
        out_shape=outs,
        in_specs=in_specs,
        out_specs=jax.tree.map(lambda _: VMEM, outs),
        scratch_shapes=scratch,
        cost_estimate=pl.CostEstimate(flops=flops, bytes_accessed=moved, transcendentals=0),
        compiler_params=pltpu.CompilerParams(vmem_limit_bytes=48 * 1024 * 1024),
        name=name,
    )


def block_offsets(blocks):
    half = max(blocks // 2, 1)
    return [2 * (b % half) + b // half for b in range(blocks)]


def order_rows(rows, blocks):
    place = lax.axis_index("tp")
    split = rows.reshape(blocks, rows.shape[0] // blocks, rows.shape[1])
    return jnp.concatenate(
        [lax.dynamic_index_in_dim(split, place ^ off, 0, keepdims=False) for off in block_offsets(blocks)]
    )


def block_copies(source, target, sems, blocks):
    rows = source.shape[0] // blocks
    if blocks == 1:
        return [pltpu.make_async_copy(source, target, sems.at[0])]
    place = lax.axis_index("tp")
    return [
        pltpu.make_async_copy(
            source.at[pl.ds(pl.multiple_of((place ^ off) * rows, ROW_TILE), rows)],
            target.at[pl.ds(b * rows, rows)],
            sems.at[b],
        )
        for b, off in enumerate(block_offsets(blocks))
    ]


def source_kernel(blocks, own, source, gain, w_key, w_value, kv, part, held, sems):
    copies = block_copies(source, held, sems, blocks)
    for copy in copies:
        copy.start()
    rows = source.shape[0]
    pieces = min(blocks, 4)
    step = rows // pieces
    per = blocks // pieces
    for piece in range(pieces):
        for copy in copies[piece * per : (piece + 1) * per]:
            copy.wait()
        span = pl.ds(piece * step, step)
        norm = normed(held[span, :], gain[...])
        kv[span, 0:HEAD] = nn(norm, w_key[...]).astype(BF16)
        kv[span, HEAD:] = nn(norm, w_value[...]).astype(BF16)
    part[...] = held[0:own, :]


def target_kernel(
    blocks, own, sp_count, target, cotangent, gain, w_query, w_out,
    q, q_t, da, da_t, part, *rest,
):
    cot_outs, (held_t, held_c, sems_t, sems_c) = rest[:sp_count], rest[sp_count:]
    copies = block_copies(cotangent, held_c, sems_c, blocks) + block_copies(
        target, held_t, sems_t, blocks
    )
    for copy in copies:
        copy.start()
    rows = target.shape[0]
    heads = w_out.shape[0] // HEAD
    for copy in copies[:blocks]:
        copy.wait()
    width = held_c.shape[1] // sp_count
    sp_place = lax.axis_index("sp")
    for k, out in enumerate(cot_outs):
        out[...] = held_c[:, pl.ds(pl.multiple_of((sp_place ^ k) * width, 128), width)]
    for h in range(heads):
        span = slice(h * HEAD, (h + 1) * HEAD)
        grad = nt(held_c[...], w_out[span, :]).astype(BF16)
        da[h * rows : (h + 1) * rows, :] = grad
        da_t[:, h * rows : (h + 1) * rows] = grad.T
    for copy in copies[blocks:]:
        copy.wait()
    norm = normed(held_t[...], gain[...])
    for h in range(heads):
        span = slice(h * HEAD, (h + 1) * HEAD)
        query = nn(norm, w_query[:, span]).astype(BF16)
        q[h * rows : (h + 1) * rows, :] = query
        q_t[:, h * rows : (h + 1) * rows] = query.T
    part[...] = held_t[0:own, :]


def attention_kernel(sp_count, q, q_t, da, da_t, *rest):
    kvs, rest = rest[:sp_count], rest[sp_count:]
    att_t, dq, keep, send, exps, prob_grads = rest
    lanes = q_t.shape[1]
    rows = dq.shape[0]
    heads = lanes // rows
    inv_root = HEAD ** (-0.5)
    group = kvs[0].shape[0]
    step = CHUNK if group % CHUNK == 0 else group // 2
    per = group // step
    half = group // 2
    total = jnp.zeros((1, lanes), F32)
    out_acc = jnp.zeros((HEAD, lanes), F32)
    for k in range(sp_count):
        for c in range(per):
            base = k * group + c * step
            key = kvs[k][c * step : (c + 1) * step, 0:HEAD]
            value = kvs[k][c * step : (c + 1) * step, HEAD:]
            exponent = jnp.exp2(nn(key, q_t[...]) * (inv_root * LOG2_E))
            total = total + jnp.sum(exponent, axis=0, keepdims=True)
            exps[base : base + step, :] = exponent
            prob_grads[base : base + step, :] = nn(value, da_t[...])
            out_acc = out_acc + nn(value.T, exponent.astype(BF16))
    inv_total = 1.0 / total
    attended = (out_acc * inv_total).astype(BF16)
    for h in range(heads):
        att_t[h * HEAD : (h + 1) * HEAD, :] = attended[:, h * rows : (h + 1) * rows]
    delta = jnp.sum(attended.astype(F32) * da_t[...].astype(F32), axis=0, keepdims=True)
    dq_acc = jnp.zeros((HEAD, lanes), F32)
    for k in range(sp_count):
        for c in range(per):
            base = k * group + c * step
            key = kvs[k][c * step : (c + 1) * step, 0:HEAD]
            probs = exps[base : base + step, :] * inv_total
            score_grad = (probs * (prob_grads[base : base + step, :] - delta)).astype(BF16)
            dkey = nn(score_grad, q[...]) * inv_root
            dvalue = nn(probs.astype(BF16), da[...])
            dq_acc = dq_acc + nn(key.T, score_grad)
            out = keep if c < per // 2 else send
            at = k * half + (c % (per // 2)) * step
            out[at : at + step, 0:HEAD] = dkey.astype(out.dtype)
            out[at : at + step, HEAD:] = dvalue.astype(out.dtype)
    dq_t = (dq_acc * inv_root).astype(BF16)
    for h in range(heads):
        dq[:, h * HEAD : (h + 1) * HEAD] = dq_t[:, h * rows : (h + 1) * rows].T


def pull_kernel(dq, w_query, keep, send):
    half = keep.shape[0]
    pulled = nt(dq[...], w_query[...])
    keep[...] = pulled[0:half]
    send[...] = pulled[half:].astype(BF16)


def fold_kernel(count, *refs):
    ins, outs = refs[:count], refs[count:]
    total = ins[0][...].astype(F32)
    for ref in ins[1:]:
        total = total + ref[...].astype(F32)
    step = total.shape[0] // len(outs)
    for b, out in enumerate(outs):
        out[...] = total[b * step : (b + 1) * step].astype(out.dtype)


def fold(parts, pieces, name):
    rows, width = parts[0].shape
    step = rows // pieces
    cut = pieces if step % ROW_TILE == 0 else 1
    outs = [shape((rows // cut, width), BF16)] * cut
    result = call(
        functools.partial(fold_kernel, len(parts)), outs, rows * width * len(parts),
        rows * width * 2 * (len(parts) + 1), [VMEM] * len(parts), name=name,
    )(*parts)
    if cut == pieces:
        return list(result)
    return [result[0][b * step : (b + 1) * step] for b in range(pieces)]


def finish_source_kernel(count, *refs):
    parts, (rows, gain, w_key, w_value, out) = refs[:count], refs[count:]
    total = parts[0][...].astype(F32)
    for ref in parts[1:]:
        total = total + ref[...].astype(F32)
    grad = total.astype(BF16)
    pulled = nt(grad[:, 0:HEAD], w_key[...]) + nt(grad[:, HEAD:], w_value[...])
    out[...] = norm_back(rows[...], gain[...], pulled).astype(BF16)


def finish_target_kernel(count, *refs):
    parts, (rows, gain, out) = refs[:count], refs[count:]
    total = parts[0][...].astype(F32)
    for ref in parts[1:]:
        total = total + ref[...].astype(F32)
    out[...] = norm_back(rows[...], gain[...], total).astype(BF16)


def grad_out_kernel(count, *refs):
    atts, cots, out = refs[:count], refs[count : 2 * count], refs[2 * count]
    total = nn(atts[0][...], cots[0][...])
    for att, cot in zip(atts[1:], cots[1:]):
        total = total + nn(att[...], cot[...])
    out[...] = total.astype(BF16)


def on_device(target, source, cotangent, target_gain, source_gain, w_query, w_key, w_value, w_out):
    tp_count, sp_count = lax.axis_size("tp"), lax.axis_size("sp")
    z_count = tp_count // 2
    t_rows, s_rows = target.shape[0], source.shape[0]
    width = target.shape[1]
    t_own, s_own = t_rows // tp_count, s_rows // tp_count
    q_width = w_query.shape[1]
    heads = q_width // HEAD
    lanes = heads * t_rows
    target_gain, source_gain = target_gain[None, :], source_gain[None, :]

    def swap(value, axis, count, offset):
        return lax.ppermute(value, axis, [(i, i ^ offset) for i in range(count)])

    def to_sp(values):
        return [values[0]] + [swap(values[k], "sp", sp_count, k) for k in range(1, sp_count)]

    def to_z(values):
        return [values[0]] + [swap(values[k], "tp", tp_count, 2 * k) for k in range(1, z_count)]

    def to_core(value):
        return swap(value, "tp", tp_count, 1)

    s_blocks = tp_count if s_own % ROW_TILE == 0 else 1
    if s_blocks == 1:
        source = order_rows(source, tp_count)
    kv, source_part = call(
        functools.partial(source_kernel, s_blocks, s_own),
        [shape((s_rows, 2 * HEAD), BF16), shape((s_own, width), BF16)],
        4 * s_rows * width * HEAD, s_rows * width * 2 + 4 * width * HEAD,
        [ANY, VMEM, VMEM, VMEM],
        [pltpu.VMEM((s_rows, width), BF16), pltpu.SemaphoreType.DMA((s_blocks,))],
        "source_rows",
    )(source, source_gain, w_key, w_value)
    kvs = to_sp([kv] * sp_count)

    t_blocks = tp_count if t_own % ROW_TILE == 0 else 1
    if t_blocks == 1:
        target, cotangent = order_rows(target, tp_count), order_rows(cotangent, tp_count)
    q, q_t, da, da_t, target_part, *cots = call(
        functools.partial(target_kernel, t_blocks, t_own, sp_count),
        [shape((lanes, HEAD), BF16), shape((HEAD, lanes), BF16)] * 2
        + [shape((t_own, width), BF16)]
        + [shape((t_rows, width // sp_count), BF16)] * sp_count,
        4 * t_rows * width * q_width, 4 * width * q_width + 4 * t_rows * width,
        [ANY, ANY, VMEM, VMEM, VMEM],
        [pltpu.VMEM((t_rows, width), BF16)] * 2 + [pltpu.SemaphoreType.DMA((t_blocks,))] * 2,
        "target_rows",
    )(target, cotangent, target_gain, w_query, w_out)
    cots = to_sp(cots)

    half = s_rows // 2
    all_rows = sp_count * s_rows
    att_t, dq, keep, send = call(
        functools.partial(attention_kernel, sp_count),
        [
            shape((q_width, t_rows), BF16),
            shape((t_rows, q_width), BF16),
            shape((sp_count * half, 2 * HEAD), F32),
            shape((sp_count * half, 2 * HEAD), BF16),
        ],
        14 * lanes * all_rows * HEAD, 4 * all_rows * HEAD + 8 * lanes * HEAD,
        [VMEM] * (4 + sp_count),
        [pltpu.VMEM((all_rows, lanes), F32)] * 2,
        "attention",
    )(q, q_t, da, da_t, *kvs)

    received = to_core(send)
    atts = to_sp([att_t] * sp_count)
    t_keep, t_send = call(
        pull_kernel,
        [shape((t_rows // 2, width), F32), shape((t_rows // 2, width), BF16)],
        2 * t_rows * width * q_width, 2 * width * q_width + 8 * t_rows * width,
        [VMEM, VMEM], (), "pull_target",
    )(dq, w_query)
    t_received = to_core(t_send)
    s_parts = to_sp(fold([keep, received], sp_count, "fold_core"))
    t_parts = to_z(fold([t_keep, t_received], z_count, "fold_target"))
    s_parts = to_z(fold(s_parts, z_count, "fold_sp"))

    grad_target = call(
        functools.partial(finish_target_kernel, z_count), shape((t_own, width), BF16),
        10 * t_own * width, 8 * t_own * width, [VMEM] * (z_count + 2), (), "finish_target",
    )(*t_parts, target_part, target_gain)
    grad_out = call(
        functools.partial(grad_out_kernel, sp_count), shape((q_width, width // sp_count), BF16),
        2 * q_width * width * t_rows, 2 * q_width * width, [VMEM] * (2 * sp_count), (), "grad_out",
    )(*atts, *cots)
    grad_source = call(
        functools.partial(finish_source_kernel, z_count), shape((s_own, width), BF16),
        4 * s_own * width * HEAD, 4 * width * HEAD, [VMEM] * (z_count + 4), (), "finish_source",
    )(*s_parts, source_part, source_gain, w_key, w_value)
    return (grad_target, grad_source, grad_out)


def solution(mesh):
    in_specs = (
        P("sp", None),
        P("sp", None),
        P("sp", None),
        P(),
        P(),
        P(None, "tp"),
        P(),
        P(),
        P("tp", None),
    )
    out_specs = (P(("sp", "tp"), None), P(("sp", "tp"), None), P("tp", "sp"))
    return jax.shard_map(
        on_device, mesh=mesh, in_specs=in_specs, out_specs=out_specs, check_vma=False
    )
```

```python
import functools

import jax
import jax.numpy as jnp
from jax import lax
from jax.experimental import pallas as pl
from jax.experimental.pallas import tpu as pltpu
from jax.sharding import PartitionSpec as P


HEAD = 128
NORM_EPS = 1e-06
LOG2_E = 1.4426950408889634
ROW_TILE = 16

BF16 = jnp.bfloat16
F32 = jnp.float32


VMEM = pl.BlockSpec(memory_space=pltpu.VMEM)
HBM = pl.BlockSpec(memory_space=pltpu.HBM)


def nn(left, right):
    return lax.dot_general(left, right, (((1,), (0,)), ((), ())), preferred_element_type=F32)


def nt(left, right):
    return lax.dot_general(left, right, (((1,), (1,)), ((), ())), preferred_element_type=F32)


def inverse_rms(rows_wide):
    return lax.rsqrt(jnp.mean(rows_wide * rows_wide, axis=1, keepdims=True) + NORM_EPS)


def norm_back(rows, gain, upstream):
    wide = rows.astype(F32)
    inv = inverse_rms(wide)
    unit = wide * inv
    pulled = upstream * gain
    return inv * (pulled - unit * jnp.mean(pulled * unit, axis=1, keepdims=True))


def in_hbm(array):
    return pltpu.with_memory_space_constraint(array, pltpu.HBM)


def shape(dims, kind):
    return jax.ShapeDtypeStruct(dims, kind)


def call(body, outs, flops, moved, in_specs, scratch=()):
    return pl.pallas_call(
        body,
        out_shape=outs,
        in_specs=in_specs,
        out_specs=jax.tree.map(lambda _: VMEM, outs),
        scratch_shapes=scratch,
        cost_estimate=pl.CostEstimate(flops=flops, bytes_accessed=moved, transcendentals=0),
        compiler_params=pltpu.CompilerParams(vmem_limit_bytes=32 * 1024 * 1024),
    )


def block_offsets(blocks):
    half = max(blocks // 2, 1)
    return [2 * (b % half) + b // half for b in range(blocks)]


def order_rows(rows, blocks):
    place = lax.axis_index("tp")
    split = rows.reshape(blocks, rows.shape[0] // blocks, rows.shape[1])
    return jnp.concatenate(
        [lax.dynamic_index_in_dim(split, place ^ off, 0, keepdims=False) for off in block_offsets(blocks)]
    )


def block_copies(source, target, sems, blocks):
    if blocks == 1:
        return [pltpu.make_async_copy(source.at[pl.ds(0, target.shape[0])], target, sems.at[0])]
    rows = source.shape[0] // blocks
    place = lax.axis_index("tp")
    return [
        pltpu.make_async_copy(
            source.at[pl.ds(pl.multiple_of((place ^ off) * rows, ROW_TILE), rows)],
            target.at[pl.ds(b * rows, rows)],
            sems.at[b],
        )
        for b, off in enumerate(block_offsets(blocks)[: target.shape[0] // rows])
    ]


def source_kernel(
    s_blocks, t_blocks, own, sp_count, source, cotangent, gain, w_key, w_value, *rest
):
    messages, rest = rest[:sp_count], rest[sp_count:]
    part, held, held_c, weights, gains, sems, c_sems, w_sems = rest
    copies = block_copies(source, held, sems, s_blocks)
    c_copies = block_copies(cotangent, held_c, c_sems, t_blocks)
    w_copies = [
        pltpu.make_async_copy(w, weights.at[:, pl.ds(n * HEAD, HEAD)], w_sems.at[n])
        for n, w in enumerate((w_key, w_value))
    ]
    w_copies.append(pltpu.make_async_copy(gain, gains, w_sems.at[2]))
    for copy in copies + w_copies + c_copies:
        copy.start()
    for copy in copies + w_copies:
        copy.wait()
    rows, c_rows = held.shape[0], held_c.shape[0]
    wide = held[...].astype(F32)
    acc = nn((wide * gains[...]).astype(BF16), weights[...])
    both = (acc * inverse_rms(wide)).astype(BF16)
    for message in messages:
        message[0:rows, :] = both[:, 0:HEAD]
        message[rows : 2 * rows, :] = both[:, HEAD:]
    part[...] = held[0:own, :]
    for copy in c_copies:
        copy.wait()
    pieces = held_c.shape[1] // (sp_count * HEAD)
    sp_place = lax.axis_index("sp")
    for k, message in enumerate(messages):
        for piece in range(pieces):
            column = pl.multiple_of(((sp_place ^ k) * pieces + piece) * HEAD, HEAD)
            at = 2 * rows + piece * c_rows
            message[at : at + c_rows, :] = held_c[:, pl.ds(column, HEAD)]


def target_kernel(
    blocks, own, target, cotangent, gain, w_query, w_out, q, q_t, da, da_t, part,
    held_t, held_c, gains, weights, sems_t, sems_c, sems,
):
    t_copies = block_copies(target, held_t, sems_t, blocks)
    c_copies = block_copies(cotangent, held_c, sems_c, blocks)
    gain_copy = pltpu.make_async_copy(gain, gains, sems.at[0])
    w_copy = pltpu.make_async_copy(w_out, weights, sems.at[1])
    for copy in t_copies + [gain_copy] + c_copies + [w_copy]:
        copy.start()
    rows = target.shape[0]
    heads = w_out.shape[0] // HEAD
    for copy in t_copies + [gain_copy]:
        copy.wait()
    wide = held_t[...].astype(F32)
    queries = nn((wide * gains[...]).astype(BF16), w_query[...])
    queries = (queries * inverse_rms(wide)).astype(BF16)
    for h in range(heads):
        query = queries[:, h * HEAD : (h + 1) * HEAD]
        q[h * rows : (h + 1) * rows, :] = query
        q_t[:, h * rows : (h + 1) * rows] = query.T
    part[...] = held_t[0:own, :]
    for copy in c_copies + [w_copy]:
        copy.wait()
    grads = nt(held_c[...], weights[...]).astype(BF16)
    for h in range(heads):
        grad = grads[:, h * HEAD : (h + 1) * HEAD]
        da[h * rows : (h + 1) * rows, :] = grad
        da_t[:, h * rows : (h + 1) * rows] = grad.T


def attend_half(half, q_t, da_t, messages, exps, prob_grads, total, out_acc):
    for k, message in enumerate(messages):
        key, value = message[0:half, :], message[half : 2 * half, :]
        exponent = jnp.exp2(nn(key, q_t[...]) * (HEAD ** (-0.5) * LOG2_E))
        total = total + jnp.sum(exponent, axis=0, keepdims=True)
        exps[k * half : (k + 1) * half, :] = exponent
        prob_grads[k * half : (k + 1) * half, :] = nn(value, da_t[...])
        out_acc = out_acc + nn(value.T, exponent.astype(BF16))
    return total, out_acc


def near_kernel(half, sp_count, q_t, da_t, *rest):
    messages, (exps, prob_grads, total, out_acc) = rest[:sp_count], rest[sp_count:]
    total[...], out_acc[...] = attend_half(
        half, q_t, da_t, messages, exps, prob_grads,
        jnp.zeros(total.shape, F32), jnp.zeros(out_acc.shape, F32),
    )


def far_kernel(half, sp_count, q, q_t, da, da_t, near_exps, near_grads, near_total, near_acc, *rest):
    near, far, rest = rest[:sp_count], rest[sp_count : 2 * sp_count], rest[2 * sp_count :]
    att_t, dq, keep, send, far_exps, far_grads = rest
    lanes = q_t.shape[1]
    rows = dq.shape[0]
    heads = lanes // rows
    inv_root = HEAD ** (-0.5)
    total, out_acc = attend_half(
        half, q_t, da_t, far, far_exps, far_grads, near_total[...], near_acc[...]
    )
    inv_total = 1.0 / total
    attended = (out_acc * inv_total).astype(BF16)
    for h in range(heads):
        att_t[h * HEAD : (h + 1) * HEAD, :] = attended[:, h * rows : (h + 1) * rows]
    delta = jnp.sum(attended.astype(F32) * da_t[...].astype(F32), axis=0, keepdims=True)
    dq_acc = jnp.zeros((HEAD, lanes), F32)
    for messages, exps, prob_grads, out in (
        (far, far_exps, far_grads, send),
        (near, near_exps, near_grads, keep),
    ):
        for k in range(sp_count):
            span = slice(k * half, (k + 1) * half)
            probs = exps[span, :] * inv_total
            score_grad = (probs * (prob_grads[span, :] - delta)).astype(BF16)
            at = 2 * k * half
            dkey = nn(score_grad, q[...]) * inv_root
            out[at : at + half, :] = dkey.astype(out.dtype)
            dvalue = nn(probs.astype(BF16), da[...])
            out[at + half : at + 2 * half, :] = dvalue.astype(out.dtype)
            dq_acc = dq_acc + nn(messages[k][0:half, :].T, score_grad)
    dq_t = (dq_acc * inv_root).astype(BF16)
    for h in range(heads):
        dq[:, h * HEAD : (h + 1) * HEAD] = dq_t[:, h * rows : (h + 1) * rows].T


def pull_kernel(dq, w_query, keep, send):
    half = keep.shape[0]
    pulled = nt(dq[...], w_query[...])
    keep[...] = pulled[0:half]
    send[...] = pulled[half:].astype(BF16)


def summed(refs, rows=slice(None)):
    total = refs[0][rows, :].astype(F32)
    for ref in refs[1:]:
        total = total + ref[rows, :].astype(F32)
    return total


def fold_core_kernel(keep, received, *outs):
    step = keep.shape[0] // len(outs)
    for b, out in enumerate(outs):
        out[...] = summed((keep, received), slice(b * step, (b + 1) * step)).astype(BF16)


def fold_sp_kernel(half, count, *refs):
    parts, outs = refs[:count], refs[count:]
    step = half // len(outs)
    for b, out in enumerate(outs):
        for part in range(2):
            at = part * half + b * step
            total = summed(parts, slice(at, at + step))
            out[part * step : (part + 1) * step, :] = total.astype(BF16)


def finish_source_kernel(count, *refs):
    parts, (rows, gain, w_key, w_value, out) = refs[:count], refs[count:]
    grad = summed(parts).astype(BF16)
    own = rows.shape[0]
    pulled = nt(grad[0:own], w_key[...]) + nt(grad[own:], w_value[...])
    out[...] = norm_back(rows[...], gain[...], pulled).astype(BF16)


def finish_target_kernel(count, *refs):
    parts, (rows, gain, out) = refs[:count], refs[count:]
    out[...] = norm_back(rows[...], gain[...], summed(parts)).astype(BF16)


def grad_out_kernel(skip_cot, count, *refs):
    atts, near, far, (out, cots) = (
        refs[:count], refs[count : 2 * count], refs[2 * count : 3 * count], refs[3 * count :]
    )
    pieces = out.shape[1] // HEAD
    rows = cots.shape[0] // 2
    total = jnp.zeros(out.shape, F32)
    for att, pair in zip(atts, zip(near, far)):
        for side, message in enumerate(pair):
            for piece in range(pieces):
                at = skip_cot + piece * rows
                cots[side * rows : (side + 1) * rows, piece * HEAD : (piece + 1) * HEAD] = message[
                    at : at + rows, :
                ]
        total = total + nn(att[...], cots[...])
    out[...] = total.astype(BF16)


def on_device(target, source, cotangent, target_gain, source_gain, w_query, w_key, w_value, w_out):
    tp_count, sp_count = lax.axis_size("tp"), lax.axis_size("sp")
    z_count = tp_count // 2
    t_rows, s_rows = target.shape[0], source.shape[0]
    width = target.shape[1]
    t_own, s_own = t_rows // tp_count, s_rows // tp_count
    q_width = w_query.shape[1]
    heads = q_width // HEAD
    lanes = heads * t_rows
    target_gain, source_gain = target_gain[None, :], source_gain[None, :]

    def swap(value, axis, count, offset):
        return lax.ppermute(value, axis, [(i, i ^ offset) for i in range(count)])

    def to_sp(values):
        return [values[0]] + [swap(values[k], "sp", sp_count, k) for k in range(1, sp_count)]

    def to_z(values):
        return [values[0]] + [swap(values[k], "tp", tp_count, 2 * k) for k in range(1, z_count)]

    def to_core(value):
        return swap(value, "tp", tp_count, 1)

    s_blocks = tp_count if s_own % ROW_TILE == 0 else 1
    t_blocks = tp_count if t_own % ROW_TILE == 0 else 1
    if s_blocks == 1:
        source = order_rows(source, tp_count)
    if t_blocks == 1:
        target, cotangent = order_rows(target, tp_count), order_rows(cotangent, tp_count)
    s_half, t_half = s_rows // 2, t_rows // 2
    far_rows = sp_count * s_half
    cot_rows = width // sp_count // HEAD * t_half

    *near, source_part = call(
        functools.partial(source_kernel, s_blocks, t_blocks, s_own, sp_count),
        [shape((2 * s_half + cot_rows, HEAD), BF16)] * sp_count + [shape((s_own, width), BF16)],
        4 * s_half * width * HEAD, s_rows * width * 2 + 4 * width * HEAD,
        [HBM] * 5,
        [
            pltpu.VMEM((s_half, width), BF16),
            pltpu.VMEM((t_half, width), BF16),
            pltpu.VMEM((width, 2 * HEAD), BF16),
            pltpu.VMEM((1, width), F32),
        ]
        + [pltpu.SemaphoreType.DMA((n,)) for n in (s_blocks, t_blocks, 3)],
    )(*map(in_hbm, (source, cotangent, source_gain, w_key, w_value)))
    near = to_sp(near)
    far = [to_core(message) for message in near]

    q, q_t, da, da_t, target_part = call(
        functools.partial(target_kernel, t_blocks, t_own),
        [shape((lanes, HEAD), BF16), shape((HEAD, lanes), BF16)] * 2
        + [shape((t_own, width), BF16)],
        4 * t_rows * width * q_width, 4 * width * q_width + 4 * t_rows * width,
        [HBM, HBM, HBM, VMEM, HBM],
        [pltpu.VMEM((t_rows, width), BF16)] * 2
        + [pltpu.VMEM((1, width), F32), pltpu.VMEM((q_width, width), BF16)]
        + [pltpu.SemaphoreType.DMA((n,)) for n in (t_blocks, t_blocks, 2)],
    )(in_hbm(target), in_hbm(cotangent), in_hbm(target_gain), w_query, in_hbm(w_out))

    stats = call(
        functools.partial(near_kernel, s_half, sp_count),
        [shape((far_rows, lanes), F32)] * 2 + [shape((1, lanes), F32), shape((HEAD, lanes), F32)],
        6 * lanes * far_rows * HEAD, 8 * far_rows * lanes,
        [VMEM] * (2 + sp_count), (),
    )(q_t, da_t, *near)
    att_t, dq, keep, send = call(
        functools.partial(far_kernel, s_half, sp_count),
        [
            shape((q_width, t_rows), BF16),
            shape((t_rows, q_width), BF16),
            shape((2 * far_rows, HEAD), F32),
            shape((2 * far_rows, HEAD), BF16),
        ],
        18 * lanes * far_rows * HEAD, 8 * far_rows * lanes,
        [VMEM] * (8 + 2 * sp_count), [pltpu.VMEM((far_rows, lanes), F32)] * 2,
    )(q, q_t, da, da_t, *stats, *near, *far)

    received = to_core(send)
    t_keep, t_send = call(
        pull_kernel,
        [shape((t_half, width), F32), shape((t_half, width), BF16)],
        2 * t_rows * width * q_width, 2 * width * q_width + 8 * t_rows * width,
        [VMEM, VMEM], (),
    )(dq, w_query)
    t_received = to_core(t_send)
    grads = call(
        fold_core_kernel, [shape((2 * s_half, HEAD), BF16)] * sp_count,
        2 * far_rows * HEAD, 16 * far_rows * HEAD, [VMEM] * 2, (),
    )(keep, received)
    atts = to_sp([att_t] * sp_count)
    grads = to_sp(grads)

    pieces = z_count if t_blocks > 1 else 1
    t_parts = call(
        fold_core_kernel, [shape((t_half // pieces, width), BF16)] * pieces,
        t_half * width, 8 * t_half * width, [VMEM] * 2, (),
    )(t_keep, t_received)
    if t_blocks == 1:
        t_parts = [t_parts[0][b * t_own : (b + 1) * t_own] for b in range(z_count)]
    t_parts = to_z(t_parts)

    pieces = z_count if s_blocks > 1 else 1
    s_parts = call(
        functools.partial(fold_sp_kernel, s_half, sp_count),
        [shape((2 * s_half // pieces, HEAD), BF16)] * pieces,
        2 * s_half * HEAD * sp_count, 16 * s_half * HEAD, [VMEM] * sp_count, (),
    )(*grads)
    if s_blocks == 1:
        both = s_parts[0].reshape(2, z_count, s_own, HEAD)
        s_parts = [both[:, b].reshape(2 * s_own, HEAD) for b in range(z_count)]
    s_parts = to_z(s_parts)

    grad_target = call(
        functools.partial(finish_target_kernel, z_count), shape((t_own, width), BF16),
        10 * t_own * width, 8 * t_own * width, [VMEM] * (z_count + 2), (),
    )(*t_parts, target_part, target_gain)
    grad_out = call(
        functools.partial(grad_out_kernel, 2 * s_half, sp_count),
        shape((q_width, width // sp_count), BF16),
        2 * q_width * width * t_rows, 2 * q_width * width, [VMEM] * (3 * sp_count),
        [pltpu.VMEM((t_rows, width // sp_count), BF16)],
    )(*atts, *near, *far)
    grad_source = call(
        functools.partial(finish_source_kernel, z_count), shape((s_own, width), BF16),
        4 * s_own * width * HEAD, 4 * width * HEAD, [VMEM] * (z_count + 4), (),
    )(*s_parts, source_part, source_gain, w_key, w_value)
    return (grad_target, grad_source, grad_out)


def solution(mesh):
    in_specs = (
        P("sp", None),
        P("sp", None),
        P("sp", None),
        P(),
        P(),
        P(None, "tp"),
        P(),
        P(),
        P("tp", None),
    )
    out_specs = (P(("sp", "tp"), None), P(("sp", "tp"), None), P("tp", "sp"))

    return jax.shard_map(
        on_device, mesh=mesh, in_specs=in_specs, out_specs=out_specs, check_vma=False
    )
```

```python
import functools

import jax
import jax.numpy as jnp
from jax import lax
from jax.experimental import pallas as pl
from jax.experimental.pallas import tpu as pltpu
from jax.sharding import PartitionSpec as P


HEAD = 128
NORM_EPS = 1e-06
LOG2_E = 1.4426950408889634
ROW_TILE = 16

BF16 = jnp.bfloat16
F32 = jnp.float32


VMEM = pl.BlockSpec(memory_space=pltpu.VMEM)
HBM = pl.BlockSpec(memory_space=pltpu.HBM)


def nn(left, right):
    return lax.dot_general(left, right, (((1,), (0,)), ((), ())), preferred_element_type=F32)


def nt(left, right):
    return lax.dot_general(left, right, (((1,), (1,)), ((), ())), preferred_element_type=F32)


def inverse_rms(rows_wide):
    return lax.rsqrt(jnp.mean(rows_wide * rows_wide, axis=1, keepdims=True) + NORM_EPS)


def norm_back(rows, gain, upstream):
    wide = rows.astype(F32)
    inv = inverse_rms(wide)
    unit = wide * inv
    pulled = upstream * gain
    return inv * (pulled - unit * jnp.mean(pulled * unit, axis=1, keepdims=True))


def in_hbm(array):
    return pltpu.with_memory_space_constraint(array, pltpu.HBM)


def shape(dims, kind):
    return jax.ShapeDtypeStruct(dims, kind)


def call(body, outs, flops, moved, in_specs, scratch=()):
    return pl.pallas_call(
        body,
        out_shape=outs,
        in_specs=in_specs,
        out_specs=jax.tree.map(lambda _: VMEM, outs),
        scratch_shapes=scratch,
        cost_estimate=pl.CostEstimate(flops=flops, bytes_accessed=moved, transcendentals=0),
        compiler_params=pltpu.CompilerParams(vmem_limit_bytes=32 * 1024 * 1024),
    )


def block_offsets(blocks):
    half = max(blocks // 2, 1)
    near = [2 * z + (z > 0) for z in range(half)]
    return (near + [off ^ 1 for off in near])[:blocks]


def order_rows(rows, blocks):
    place = lax.axis_index("tp")
    split = rows.reshape(blocks, rows.shape[0] // blocks, rows.shape[1])
    return jnp.concatenate(
        [lax.dynamic_index_in_dim(split, place ^ off, 0, keepdims=False) for off in block_offsets(blocks)]
    )


def block_copies(source, target, sems, blocks):
    if blocks == 1:
        return [pltpu.make_async_copy(source.at[pl.ds(0, target.shape[0])], target, sems.at[0])]
    rows = source.shape[0] // blocks
    place = lax.axis_index("tp")
    return [
        pltpu.make_async_copy(
            source.at[pl.ds(pl.multiple_of((place ^ off) * rows, ROW_TILE), rows)],
            target.at[pl.ds(b * rows, rows)],
            sems.at[b],
        )
        for b, off in enumerate(block_offsets(blocks)[: target.shape[0] // rows])
    ]


def source_kernel(blocks, own, source, gain, w_key, w_value, *rest):
    message, part, held, weights, gains, sems, w_sems = rest
    copies = block_copies(source, held, sems, blocks)
    copies += [
        pltpu.make_async_copy(w, weights.at[:, pl.ds(n * HEAD, HEAD)], w_sems.at[n])
        for n, w in enumerate((w_key, w_value))
    ]
    copies.append(pltpu.make_async_copy(gain, gains, w_sems.at[2]))
    for copy in copies:
        copy.start()
    for copy in copies:
        copy.wait()
    rows = held.shape[0]
    wide = held[...].astype(F32)
    acc = nn((wide * gains[...]).astype(BF16), weights[...])
    both = (acc * inverse_rms(wide)).astype(BF16)
    message[0:rows, :] = both[:, 0:HEAD]
    message[rows:, :] = both[:, HEAD:]
    part[...] = held[0:own, :]


def target_kernel(
    blocks, own, sp_count, target, cotangent, gain, w_query, w_out, q, q_t, da, da_t, part, *rest
):
    cots, rest = rest[:sp_count], rest[sp_count:]
    held_t, held_c, gains, weights, sems_t, sems_c, sems = rest
    t_copies = block_copies(target, held_t, sems_t, blocks)
    c_copies = block_copies(cotangent, held_c, sems_c, blocks)
    gain_copy = pltpu.make_async_copy(gain, gains, sems.at[0])
    w_copy = pltpu.make_async_copy(w_out, weights, sems.at[1])
    for copy in t_copies + [gain_copy] + c_copies + [w_copy]:
        copy.start()
    rows = target.shape[0]
    heads = w_out.shape[0] // HEAD
    for copy in t_copies + [gain_copy]:
        copy.wait()
    wide = held_t[...].astype(F32)
    queries = nn((wide * gains[...]).astype(BF16), w_query[...])
    queries = (queries * inverse_rms(wide)).astype(BF16)
    for h in range(heads):
        query = queries[:, h * HEAD : (h + 1) * HEAD]
        q[h * rows : (h + 1) * rows, :] = query
        q_t[:, h * rows : (h + 1) * rows] = query.T
    part[...] = held_t[0:own, :]
    for copy in c_copies + [w_copy]:
        copy.wait()
    pieces = held_c.shape[1] // (sp_count * HEAD)
    sp_place = lax.axis_index("sp")
    for k, cot in enumerate(cots):
        for piece in range(pieces):
            column = pl.multiple_of(((sp_place ^ k) * pieces + piece) * HEAD, HEAD)
            cot[piece * rows // 2 : (piece + 1) * rows // 2, :] = held_c[
                0 : rows // 2, pl.ds(column, HEAD)
            ]
    grads = nt(held_c[...], weights[...]).astype(BF16)
    for h in range(heads):
        grad = grads[:, h * HEAD : (h + 1) * HEAD]
        da[h * rows : (h + 1) * rows, :] = grad
        da_t[:, h * rows : (h + 1) * rows] = grad.T


def attend_half(half, q_t, da_t, messages, exps, prob_grads, total, out_acc):
    for k, message in enumerate(messages):
        key, value = message[0:half, :], message[half : 2 * half, :]
        exponent = jnp.exp2(nn(key, q_t[...]) * (HEAD ** (-0.5) * LOG2_E))
        total = total + jnp.sum(exponent, axis=0, keepdims=True)
        exps[k * half : (k + 1) * half, :] = exponent
        prob_grads[k * half : (k + 1) * half, :] = nn(value, da_t[...])
        out_acc = out_acc + nn(value.T, exponent.astype(BF16))
    return total, out_acc


def near_kernel(half, sp_count, q_t, da_t, *rest):
    messages, (exps, prob_grads, total, out_acc) = rest[:sp_count], rest[sp_count:]
    total[...], out_acc[...] = attend_half(
        half, q_t, da_t, messages, exps, prob_grads,
        jnp.zeros(total.shape, F32), jnp.zeros(out_acc.shape, F32),
    )


def far_kernel(half, sp_count, q, q_t, da, da_t, near_exps, near_grads, near_total, near_acc, *rest):
    near, far, rest = rest[:sp_count], rest[sp_count : 2 * sp_count], rest[2 * sp_count :]
    att_t, dq, keep, send, far_exps, far_grads = rest
    lanes = q_t.shape[1]
    rows = dq.shape[0]
    heads = lanes // rows
    inv_root = HEAD ** (-0.5)
    total, out_acc = attend_half(
        half, q_t, da_t, far, far_exps, far_grads, near_total[...], near_acc[...]
    )
    inv_total = 1.0 / total
    attended = (out_acc * inv_total).astype(BF16)
    for h in range(heads):
        att_t[h * HEAD : (h + 1) * HEAD, :] = attended[:, h * rows : (h + 1) * rows]
    delta = jnp.sum(attended.astype(F32) * da_t[...].astype(F32), axis=0, keepdims=True)
    dq_acc = jnp.zeros((HEAD, lanes), F32)
    for messages, exps, prob_grads, out in (
        (far, far_exps, far_grads, send),
        (near, near_exps, near_grads, keep),
    ):
        for k in range(sp_count):
            span = slice(k * half, (k + 1) * half)
            probs = exps[span, :] * inv_total
            score_grad = (probs * (prob_grads[span, :] - delta)).astype(BF16)
            at = 2 * k * half
            dkey = nn(score_grad, q[...]) * inv_root
            out[at : at + half, :] = dkey.astype(out.dtype)
            dvalue = nn(probs.astype(BF16), da[...])
            out[at + half : at + 2 * half, :] = dvalue.astype(out.dtype)
            dq_acc = dq_acc + nn(messages[k][0:half, :].T, score_grad)
    dq_t = (dq_acc * inv_root).astype(BF16)
    for h in range(heads):
        dq[:, h * HEAD : (h + 1) * HEAD] = dq_t[:, h * rows : (h + 1) * rows].T


def pull_kernel(dq, w_query, keep, send):
    half = keep.shape[0]
    pulled = nt(dq[...], w_query[...])
    keep[...] = pulled[0:half]
    send[...] = pulled[half:].astype(BF16)


def summed(refs, rows=slice(None)):
    total = refs[0][rows, :].astype(F32)
    for ref in refs[1:]:
        total = total + ref[rows, :].astype(F32)
    return total


def fold_core_kernel(keep, received, *refs):
    count = len(refs) // 2
    for k, (cot, message) in enumerate(zip(refs[:count], refs[count:])):
        rows = message.shape[0] - cot.shape[0]
        span = slice(k * rows, (k + 1) * rows)
        message[0:rows, :] = summed((keep, received), span).astype(BF16)
        message[rows:, :] = cot[...]


def fold_target_kernel(keep, received, *outs):
    step = keep.shape[0] // len(outs)
    for b, out in enumerate(outs):
        out[...] = summed((keep, received), slice(b * step, (b + 1) * step)).astype(BF16)


def fold_sp_kernel(half, count, *refs):
    messages, cots, outs = refs[:count], refs[count], refs[count + 1 :]
    step = half // len(outs)
    for b, out in enumerate(outs):
        for part in range(2):
            at = part * half + b * step
            total = summed(messages, slice(at, at + step))
            out[part * step : (part + 1) * step, :] = total.astype(BF16)
    rows = cots.shape[0] // count
    for k, message in enumerate(messages):
        cots[k * rows : (k + 1) * rows, :] = message[2 * half :, :]


def finish_source_kernel(count, *refs):
    parts, (rows, gain, w_key, w_value, out) = refs[:count], refs[count:]
    grad = summed(parts).astype(BF16)
    own = rows.shape[0]
    pulled = nt(grad[0:own], w_key[...]) + nt(grad[own:], w_value[...])
    out[...] = norm_back(rows[...], gain[...], pulled).astype(BF16)


def finish_target_kernel(count, z_count, *refs):
    parts, (part, gain), refs = refs[:z_count], refs[z_count : z_count + 2], refs[z_count + 2 :]
    atts, (near, far, grad_target, grad_out, cots) = refs[:count], refs[count:]
    grad_target[...] = norm_back(part[...], gain[...], summed(parts)).astype(BF16)
    pieces = grad_out.shape[1] // HEAD
    rows = cots.shape[0] // 2
    total = jnp.zeros(grad_out.shape, F32)
    for k, att in enumerate(atts):
        first, second = (near, far) if k == 0 else (far, near)
        for piece in range(pieces):
            at = (k * pieces + piece) * rows
            column = slice(piece * HEAD, (piece + 1) * HEAD)
            cots[0:rows, column] = first[at : at + rows, :]
            cots[rows:, column] = second[at : at + rows, :]
        total = total + nn(att[...], cots[...])
    grad_out[...] = total.astype(BF16)


def on_device(target, source, cotangent, target_gain, source_gain, w_query, w_key, w_value, w_out):
    tp_count, sp_count = lax.axis_size("tp"), lax.axis_size("sp")
    z_count = tp_count // 2
    t_rows, s_rows = target.shape[0], source.shape[0]
    width = target.shape[1]
    t_own, s_own = t_rows // tp_count, s_rows // tp_count
    q_width = w_query.shape[1]
    heads = q_width // HEAD
    lanes = heads * t_rows
    target_gain, source_gain = target_gain[None, :], source_gain[None, :]

    def swap(value, sp_offset, tp_offset):
        pairs = [
            (s * tp_count + t, (s ^ sp_offset) * tp_count + (t ^ tp_offset))
            for s in range(sp_count)
            for t in range(tp_count)
        ]
        return lax.ppermute(value, ("sp", "tp"), pairs)

    def to_sp(values, other_core):
        return [values[0]] + [swap(values[k], k, other_core) for k in range(1, sp_count)]

    def to_z(values):
        return [values[0]] + [swap(values[k], 0, 2 * k + 1) for k in range(1, z_count)]

    def to_core(value):
        return swap(value, 0, 1)

    s_blocks = tp_count if s_own % ROW_TILE == 0 else 1
    t_blocks = tp_count if t_own % ROW_TILE == 0 else 1
    if s_blocks == 1:
        source = order_rows(source, tp_count)
    if t_blocks == 1:
        target, cotangent = order_rows(target, tp_count), order_rows(cotangent, tp_count)
    s_half, t_half = s_rows // 2, t_rows // 2
    far_rows = sp_count * s_half
    cot_rows = width // sp_count // HEAD * t_half

    message, source_part = call(
        functools.partial(source_kernel, s_blocks, s_own),
        [shape((2 * s_half, HEAD), BF16), shape((s_own, width), BF16)],
        4 * s_half * width * HEAD, s_rows * width * 2 + 4 * width * HEAD,
        [HBM] * 4,
        [
            pltpu.VMEM((s_half, width), BF16),
            pltpu.VMEM((width, 2 * HEAD), BF16),
            pltpu.VMEM((1, width), F32),
            pltpu.SemaphoreType.DMA((s_blocks,)),
            pltpu.SemaphoreType.DMA((3,)),
        ],
    )(*map(in_hbm, (source, source_gain, w_key, w_value)))
    near = to_sp([message] * sp_count, 1)
    far = [to_core(message) for message in near]

    q, q_t, da, da_t, target_part, *cots = call(
        functools.partial(target_kernel, t_blocks, t_own, sp_count),
        [shape((lanes, HEAD), BF16), shape((HEAD, lanes), BF16)] * 2
        + [shape((t_own, width), BF16)]
        + [shape((cot_rows, HEAD), BF16)] * sp_count,
        4 * t_rows * width * q_width, 4 * width * q_width + 4 * t_rows * width,
        [HBM, HBM, HBM, VMEM, HBM],
        [pltpu.VMEM((t_rows, width), BF16)] * 2
        + [pltpu.VMEM((1, width), F32), pltpu.VMEM((q_width, width), BF16)]
        + [pltpu.SemaphoreType.DMA((n,)) for n in (t_blocks, t_blocks, 2)],
    )(in_hbm(target), in_hbm(cotangent), in_hbm(target_gain), w_query, in_hbm(w_out))

    stats = call(
        functools.partial(near_kernel, s_half, sp_count),
        [shape((far_rows, lanes), F32)] * 2 + [shape((1, lanes), F32), shape((HEAD, lanes), F32)],
        6 * lanes * far_rows * HEAD, 8 * far_rows * lanes,
        [VMEM] * (2 + sp_count), (),
    )(q_t, da_t, *near)
    att_t, dq, keep, send = call(
        functools.partial(far_kernel, s_half, sp_count),
        [
            shape((q_width, t_rows), BF16),
            shape((t_rows, q_width), BF16),
            shape((2 * far_rows, HEAD), F32),
            shape((2 * far_rows, HEAD), BF16),
        ],
        18 * lanes * far_rows * HEAD, 8 * far_rows * lanes,
        [VMEM] * (8 + 2 * sp_count), [pltpu.VMEM((far_rows, lanes), F32)] * 2,
    )(q, q_t, da, da_t, *stats, *near, *far)

    received = to_core(send)
    t_keep, t_send = call(
        pull_kernel,
        [shape((t_half, width), F32), shape((t_half, width), BF16)],
        2 * t_rows * width * q_width, 2 * width * q_width + 8 * t_rows * width,
        [VMEM, VMEM], (),
    )(dq, w_query)
    t_received = to_core(t_send)
    messages = call(
        fold_core_kernel, [shape((2 * s_half + cot_rows, HEAD), BF16)] * sp_count,
        2 * far_rows * HEAD, 16 * far_rows * HEAD, [VMEM] * (2 + sp_count), (),
    )(keep, received, *cots)
    messages = to_sp(messages, 1)
    atts = to_sp([att_t] * sp_count, 0)

    pieces = z_count if t_blocks > 1 else 1
    t_parts = call(
        fold_target_kernel, [shape((t_half // pieces, width), BF16)] * pieces,
        t_half * width, 8 * t_half * width, [VMEM] * 2, (),
    )(t_keep, t_received)
    if t_blocks == 1:
        t_parts = [t_parts[0][b * t_own : (b + 1) * t_own] for b in range(z_count)]
    t_parts = to_z(t_parts)

    pieces = z_count if s_blocks > 1 else 1
    cots, *s_parts = call(
        functools.partial(fold_sp_kernel, s_half, sp_count),
        [shape((sp_count * cot_rows, HEAD), BF16)]
        + [shape((2 * s_half // pieces, HEAD), BF16)] * pieces,
        2 * s_half * HEAD * sp_count, 16 * s_half * HEAD, [VMEM] * sp_count, (),
    )(*messages)
    if s_blocks == 1:
        both = s_parts[0].reshape(2, z_count, s_own, HEAD)
        s_parts = [both[:, b].reshape(2 * s_own, HEAD) for b in range(z_count)]
    s_parts = to_z(s_parts)
    far_cots = to_core(cots)

    grad_target, grad_out = call(
        functools.partial(finish_target_kernel, sp_count, z_count),
        [shape((t_own, width), BF16), shape((q_width, width // sp_count), BF16)],
        2 * q_width * width * t_rows, 2 * q_width * width, [VMEM] * (z_count + sp_count + 4),
        [pltpu.VMEM((t_rows, width // sp_count), BF16)],
    )(*t_parts, target_part, target_gain, *atts, cots, far_cots)
    grad_source = call(
        functools.partial(finish_source_kernel, z_count), shape((s_own, width), BF16),
        4 * s_own * width * HEAD, 4 * width * HEAD, [VMEM] * (z_count + 4), (),
    )(*s_parts, source_part, source_gain, w_key, w_value)
    return (grad_target, grad_source, grad_out)


def solution(mesh):
    in_specs = (
        P("sp", None),
        P("sp", None),
        P("sp", None),
        P(),
        P(),
        P(None, "tp"),
        P(),
        P(),
        P("tp", None),
    )
    out_specs = (P(("sp", "tp"), None), P(("sp", "tp"), None), P("tp", "sp"))

    return jax.shard_map(
        on_device, mesh=mesh, in_specs=in_specs, out_specs=out_specs, check_vma=False
    )
```

```python
import functools

import jax
import jax.numpy as jnp
from jax import lax
from jax.experimental import pallas as pl
from jax.experimental.pallas import tpu as pltpu
from jax.sharding import PartitionSpec as P


HEAD = 128
NORM_EPS = 1e-06
LOG2_E = 1.4426950408889634
ROW_TILE = 16
DEPTH = 256

BF16 = jnp.bfloat16
F32 = jnp.float32


VMEM = pl.BlockSpec(memory_space=pltpu.VMEM)
HBM = pl.BlockSpec(memory_space=pltpu.HBM)


def nn(left, right):
    return lax.dot_general(left, right, (((1,), (0,)), ((), ())), preferred_element_type=F32)


def nt(left, right):
    return lax.dot_general(left, right, (((1,), (1,)), ((), ())), preferred_element_type=F32)


def inverse_rms(rows_wide):
    return lax.rsqrt(jnp.mean(rows_wide * rows_wide, axis=1, keepdims=True) + NORM_EPS)


def norm_back(rows, gain, upstream):
    wide = rows.astype(F32)
    inv = inverse_rms(wide)
    unit = wide * inv
    pulled = upstream * gain
    return inv * (pulled - unit * jnp.mean(pulled * unit, axis=1, keepdims=True))


def in_hbm(array):
    return pltpu.with_memory_space_constraint(array, pltpu.HBM)


def shape(dims, kind):
    return jax.ShapeDtypeStruct(dims, kind)


def call(body, outs, flops, moved, in_specs, scratch=()):
    return pl.pallas_call(
        body,
        out_shape=outs,
        in_specs=in_specs,
        out_specs=jax.tree.map(lambda _: VMEM, outs),
        scratch_shapes=scratch,
        cost_estimate=pl.CostEstimate(flops=flops, bytes_accessed=moved, transcendentals=0),
        compiler_params=pltpu.CompilerParams(vmem_limit_bytes=32 * 1024 * 1024),
    )


def block_offsets(blocks):
    half = max(blocks // 2, 1)
    near = [2 * z + (z > 0) for z in range(half)]
    return (near + [off ^ 1 for off in near])[:blocks]


def order_rows(rows, blocks):
    place = lax.axis_index("tp")
    split = rows.reshape(blocks, rows.shape[0] // blocks, rows.shape[1])
    return jnp.concatenate(
        [lax.dynamic_index_in_dim(split, place ^ off, 0, keepdims=False) for off in block_offsets(blocks)]
    )


def block_copies(source, target, sems, blocks):
    if blocks == 1:
        return [pltpu.make_async_copy(source.at[pl.ds(0, target.shape[0])], target, sems.at[0])]
    rows = source.shape[0] // blocks
    place = lax.axis_index("tp")
    return [
        pltpu.make_async_copy(
            source.at[pl.ds(pl.multiple_of((place ^ off) * rows, ROW_TILE), rows)],
            target.at[pl.ds(b * rows, rows)],
            sems.at[b],
        )
        for b, off in enumerate(block_offsets(blocks)[: target.shape[0] // rows])
    ]


def source_kernel(blocks, own, source, gain, w_key, w_value, *rest):
    message, part, held, weights, gains, sems, w_sems = rest
    copies = block_copies(source, held, sems, blocks)
    copies += [
        pltpu.make_async_copy(w, weights.at[:, pl.ds(n * HEAD, HEAD)], w_sems.at[n])
        for n, w in enumerate((w_key, w_value))
    ]
    copies.append(pltpu.make_async_copy(gain, gains, w_sems.at[2]))
    for copy in copies:
        copy.start()
    for copy in copies:
        copy.wait()
    rows = held.shape[0]
    wide = held[...].astype(F32)
    acc = nn((wide * gains[...]).astype(BF16), weights[...])
    both = (acc * inverse_rms(wide)).astype(BF16)
    message[0:rows, :] = both[:, 0:HEAD]
    message[rows:, :] = both[:, HEAD:]
    part[...] = held[0:own, :]


def target_kernel(
    blocks, own, sp_count, target, cotangent, gain, w_query, w_out, q, q_t, da, da_t, part, *rest
):
    cots, rest = rest[:sp_count], rest[sp_count:]
    held_t, held_c, gains, weights, sems_t, sems_c, sems = rest
    t_copies = block_copies(target, held_t, sems_t, blocks)
    c_copies = block_copies(cotangent, held_c, sems_c, blocks)
    gain_copy = pltpu.make_async_copy(gain, gains, sems.at[0])
    w_copy = pltpu.make_async_copy(w_out, weights, sems.at[1])
    for copy in t_copies + [gain_copy] + c_copies + [w_copy]:
        copy.start()
    rows = target.shape[0]
    heads = w_out.shape[0] // HEAD
    for copy in t_copies + [gain_copy]:
        copy.wait()
    wide = held_t[...].astype(F32)
    queries = nn((wide * gains[...]).astype(BF16), w_query[...])
    queries = (queries * inverse_rms(wide)).astype(BF16)
    for h in range(heads):
        query = queries[:, h * HEAD : (h + 1) * HEAD]
        q[h * rows : (h + 1) * rows, :] = query
        q_t[:, h * rows : (h + 1) * rows] = query.T
    part[...] = held_t[0:own, :]
    for copy in c_copies + [w_copy]:
        copy.wait()
    pieces = held_c.shape[1] // (sp_count * HEAD)
    sp_place = lax.axis_index("sp")
    for k, cot in enumerate(cots):
        for piece in range(pieces):
            column = pl.multiple_of(((sp_place ^ k) * pieces + piece) * HEAD, HEAD)
            cot[piece * rows // 2 : (piece + 1) * rows // 2, :] = held_c[
                0 : rows // 2, pl.ds(column, HEAD)
            ]
    grads = nt(held_c[...], weights[...]).astype(BF16)
    for h in range(heads):
        grad = grads[:, h * HEAD : (h + 1) * HEAD]
        da[h * rows : (h + 1) * rows, :] = grad
        da_t[:, h * rows : (h + 1) * rows] = grad.T


def joined(messages, half, part):
    return jnp.concatenate([m[part * half : (part + 1) * half, :] for m in messages])


def chunk_spans(rows, half):
    step = DEPTH if rows % DEPTH == 0 else half
    return [slice(at, at + step) for at in range(0, rows, step)]


def attend(half, q_t, da_t, messages, exps, prob_grads, total, out_acc):
    keys, values = joined(messages, half, 0), joined(messages, half, 1)
    for span in chunk_spans(keys.shape[0], half):
        exponent = jnp.exp2(nn(keys[span], q_t[...]) * (HEAD ** (-0.5) * LOG2_E))
        total = total + jnp.sum(exponent, axis=0, keepdims=True)
        exps[span, :] = exponent
        prob_grads[span, :] = nn(values[span], da_t[...])
        out_acc = out_acc + nn(values[span].T, exponent.astype(BF16))
    return total, out_acc


def pull_back(half, q, da, messages, exps, prob_grads, inv_total, delta, out):
    inv_root = HEAD ** (-0.5)
    keys = joined(messages, half, 0)
    rows = keys.shape[0]
    acc = jnp.zeros((HEAD, q.shape[0]), F32)
    for span in chunk_spans(rows, half):
        probs = exps[span, :] * inv_total
        score_grad = (probs * (prob_grads[span, :] - delta)).astype(BF16)
        dkey = nn(score_grad, q[...]) * inv_root
        out[span, :] = dkey.astype(out.dtype)
        dvalue = nn(probs.astype(BF16), da[...])
        out[rows + span.start : rows + span.stop, :] = dvalue.astype(out.dtype)
        acc = acc + nn(keys[span].T, score_grad)
    return acc


def near_kernel(half, sp_count, q_t, da_t, *rest):
    messages, (exps, prob_grads, total, out_acc) = rest[:sp_count], rest[sp_count:]
    total[...], out_acc[...] = attend(
        half, q_t, da_t, messages, exps, prob_grads,
        jnp.zeros(total.shape, F32), jnp.zeros(out_acc.shape, F32),
    )


def far_kernel(half, sp_count, q, q_t, da, da_t, near_total, near_acc, *rest):
    far, rest = rest[:sp_count], rest[sp_count:]
    att_t, send, inv_totals, deltas, dq_acc, exps, prob_grads = rest
    lanes, rows = q_t.shape[1], att_t.shape[1]
    total, out_acc = attend(
        half, q_t, da_t, far, exps, prob_grads, near_total[...], near_acc[...]
    )
    inv_total = 1.0 / total
    attended = (out_acc * inv_total).astype(BF16)
    for h in range(lanes // rows):
        att_t[h * HEAD : (h + 1) * HEAD, :] = attended[:, h * rows : (h + 1) * rows]
    delta = jnp.sum(attended.astype(F32) * da_t[...].astype(F32), axis=0, keepdims=True)
    inv_totals[...] = inv_total
    deltas[...] = delta
    dq_acc[...] = pull_back(half, q, da, far, exps, prob_grads, inv_total, delta, send)


def back_kernel(half, sp_count, q, da, exps, prob_grads, inv_totals, deltas, dq_acc, w_query, *rest):
    near, (keep, t_keep, t_send, dq) = rest[:sp_count], rest[sp_count:]
    rows = dq.shape[0]
    acc = dq_acc[...] + pull_back(
        half, q, da, near, exps, prob_grads, inv_totals[...], deltas[...], keep
    )
    dq_t = (acc * HEAD ** (-0.5)).astype(BF16)
    for h in range(dq_t.shape[1] // rows):
        dq[:, h * HEAD : (h + 1) * HEAD] = dq_t[:, h * rows : (h + 1) * rows].T
    pulled = nt(dq[...], w_query[...])
    t_keep[...] = pulled[0 : rows // 2]
    t_send[...] = pulled[rows // 2 :].astype(BF16)


def summed(refs, rows=slice(None)):
    total = refs[0][rows, :].astype(F32)
    for ref in refs[1:]:
        total = total + ref[rows, :].astype(F32)
    return total


def fold_core_kernel(keep, received, *refs):
    count = len(refs) // 2
    for k, (cot, message) in enumerate(zip(refs[:count], refs[count:])):
        half = (message.shape[0] - cot.shape[0]) // 2
        for part in range(2):
            at = (part * count + k) * half
            total = summed((keep, received), slice(at, at + half))
            message[part * half : (part + 1) * half, :] = total.astype(BF16)
        message[2 * half :, :] = cot[...]


def fold_target_kernel(keep, received, *outs):
    step = keep.shape[0] // len(outs)
    for b, out in enumerate(outs):
        out[...] = summed((keep, received), slice(b * step, (b + 1) * step)).astype(BF16)


def fold_sp_kernel(half, count, *refs):
    messages, cots, outs = refs[:count], refs[count], refs[count + 1 :]
    step = half // len(outs)
    for b, out in enumerate(outs):
        for part in range(2):
            at = part * half + b * step
            total = summed(messages, slice(at, at + step))
            out[part * step : (part + 1) * step, :] = total.astype(BF16)
    rows = cots.shape[0] // count
    for k, message in enumerate(messages):
        cots[k * rows : (k + 1) * rows, :] = message[2 * half :, :]


def prepare_kernel(rows, gain, w_key, w_value, unit, gained, inv, weights):
    wide = rows[...].astype(F32)
    inv_rms = inverse_rms(wide)
    inv[...] = jnp.broadcast_to(inv_rms, inv.shape)
    unit[...] = wide * inv_rms
    gained[...] = wide * inv_rms * gain[...]
    weights[0:HEAD, :] = w_key[...].T
    weights[HEAD:, :] = w_value[...].T


def finish_source_kernel(count, *refs):
    parts, (unit, gained, inv, gain, weights, out) = refs[:count], refs[count:]
    grad = summed(parts).astype(BF16)
    own = unit.shape[0]
    both = jnp.concatenate([grad[0:own], grad[own:]], axis=1)
    pulled = nn(both, weights[...])
    mean = jnp.mean(pulled * gained[...], axis=1, keepdims=True)
    out[...] = (inv[:, 0:1] * (pulled * gain[...] - unit[...] * mean)).astype(BF16)


def finish_target_kernel(count, z_count, *refs):
    parts, (part, gain), refs = refs[:z_count], refs[z_count : z_count + 2], refs[z_count + 2 :]
    atts, (near, far, grad_target, grad_out, cots, att_all) = refs[:count], refs[count:]
    grad_target[...] = norm_back(part[...], gain[...], summed(parts)).astype(BF16)
    pieces = grad_out.shape[1] // HEAD
    rows = cots.shape[0] // (2 * count)
    for k, att in enumerate(atts):
        first, second = (near, far) if k == 0 else (far, near)
        for piece in range(pieces):
            at = (k * pieces + piece) * rows
            column = slice(piece * HEAD, (piece + 1) * HEAD)
            top = 2 * k * rows
            cots[top : top + rows, column] = first[at : at + rows, :]
            cots[top + rows : top + 2 * rows, column] = second[at : at + rows, :]
        att_all[:, 2 * k * rows : 2 * (k + 1) * rows] = att[...]
    grad_out[...] = nn(att_all[...], cots[...]).astype(BF16)


def on_device(target, source, cotangent, target_gain, source_gain, w_query, w_key, w_value, w_out):
    tp_count, sp_count = lax.axis_size("tp"), lax.axis_size("sp")
    z_count = tp_count // 2
    t_rows, s_rows = target.shape[0], source.shape[0]
    width = target.shape[1]
    t_own, s_own = t_rows // tp_count, s_rows // tp_count
    q_width = w_query.shape[1]
    heads = q_width // HEAD
    lanes = heads * t_rows
    target_gain, source_gain = target_gain[None, :], source_gain[None, :]

    def swap(value, sp_offset, tp_offset):
        pairs = [
            (s * tp_count + t, (s ^ sp_offset) * tp_count + (t ^ tp_offset))
            for s in range(sp_count)
            for t in range(tp_count)
        ]
        return lax.ppermute(value, ("sp", "tp"), pairs)

    def to_sp(values, other_core):
        return [values[0]] + [swap(values[k], k, other_core) for k in range(1, sp_count)]

    def to_z(values):
        return [values[0]] + [swap(values[k], 0, 2 * k + 1) for k in range(1, z_count)]

    def to_core(value):
        return swap(value, 0, 1)

    s_blocks = tp_count if s_own % ROW_TILE == 0 else 1
    t_blocks = tp_count if t_own % ROW_TILE == 0 else 1
    if s_blocks == 1:
        source = order_rows(source, tp_count)
    if t_blocks == 1:
        target, cotangent = order_rows(target, tp_count), order_rows(cotangent, tp_count)
    s_half, t_half = s_rows // 2, t_rows // 2
    far_rows = sp_count * s_half
    cot_rows = width // sp_count // HEAD * t_half

    message, source_part = call(
        functools.partial(source_kernel, s_blocks, s_own),
        [shape((2 * s_half, HEAD), BF16), shape((s_own, width), BF16)],
        4 * s_half * width * HEAD, s_rows * width * 2 + 4 * width * HEAD,
        [HBM] * 4,
        [
            pltpu.VMEM((s_half, width), BF16),
            pltpu.VMEM((width, 2 * HEAD), BF16),
            pltpu.VMEM((1, width), F32),
            pltpu.SemaphoreType.DMA((s_blocks,)),
            pltpu.SemaphoreType.DMA((3,)),
        ],
    )(*map(in_hbm, (source, source_gain, w_key, w_value)))
    near = to_sp([message] * sp_count, 1)
    far = [to_core(message) for message in near]

    q, q_t, da, da_t, target_part, *cots = call(
        functools.partial(target_kernel, t_blocks, t_own, sp_count),
        [shape((lanes, HEAD), BF16), shape((HEAD, lanes), BF16)] * 2
        + [shape((t_own, width), BF16)]
        + [shape((cot_rows, HEAD), BF16)] * sp_count,
        4 * t_rows * width * q_width, 4 * width * q_width + 4 * t_rows * width,
        [HBM, HBM, HBM, VMEM, HBM],
        [pltpu.VMEM((t_rows, width), BF16)] * 2
        + [pltpu.VMEM((1, width), F32), pltpu.VMEM((q_width, width), BF16)]
        + [pltpu.SemaphoreType.DMA((n,)) for n in (t_blocks, t_blocks, 2)],
    )(in_hbm(target), in_hbm(cotangent), in_hbm(target_gain), w_query, in_hbm(w_out))

    unit, gained, inv, weights = call(
        prepare_kernel,
        [shape((s_own, width), F32)] * 2
        + [shape((s_own, HEAD), F32), shape((2 * HEAD, width), BF16)],
        8 * s_own * width, 8 * width * HEAD, [VMEM] * 4, (),
    )(source_part, source_gain, w_key, w_value)
    prepared = (unit, gained, inv, source_gain, weights)

    stats = call(
        functools.partial(near_kernel, s_half, sp_count),
        [shape((far_rows, lanes), F32)] * 2 + [shape((1, lanes), F32), shape((HEAD, lanes), F32)],
        6 * lanes * far_rows * HEAD, 8 * far_rows * lanes,
        [VMEM] * (2 + sp_count), (),
    )(q_t, da_t, *near)
    exps, prob_grads, total, out_acc = stats
    att_t, send, inv_total, delta, dq_acc = call(
        functools.partial(far_kernel, s_half, sp_count),
        [
            shape((q_width, t_rows), BF16),
            shape((2 * far_rows, HEAD), BF16),
            shape((1, lanes), F32),
            shape((1, lanes), F32),
            shape((HEAD, lanes), F32),
        ],
        12 * lanes * far_rows * HEAD, 8 * far_rows * lanes,
        [VMEM] * (6 + sp_count), [pltpu.VMEM((far_rows, lanes), F32)] * 2,
    )(q, q_t, da, da_t, total, out_acc, *far)
    received = to_core(send)
    keep, t_keep, t_send = call(
        functools.partial(back_kernel, s_half, sp_count),
        [
            shape((2 * far_rows, HEAD), F32),
            shape((t_half, width), F32),
            shape((t_half, width), BF16),
        ],
        6 * lanes * far_rows * HEAD + 2 * t_rows * width * q_width,
        8 * far_rows * lanes + 2 * width * q_width,
        [VMEM] * (8 + sp_count), [pltpu.VMEM((t_rows, q_width), BF16)],
    )(q, da, exps, prob_grads, inv_total, delta, dq_acc, w_query, *near)
    t_received = to_core(t_send)
    messages = call(
        fold_core_kernel, [shape((2 * s_half + cot_rows, HEAD), BF16)] * sp_count,
        2 * far_rows * HEAD, 16 * far_rows * HEAD, [VMEM] * (2 + sp_count), (),
    )(keep, received, *cots)
    messages = to_sp(messages, 1)
    atts = to_sp([att_t] * sp_count, 0)

    pieces = z_count if t_blocks > 1 else 1
    t_parts = call(
        fold_target_kernel, [shape((t_half // pieces, width), BF16)] * pieces,
        t_half * width, 8 * t_half * width, [VMEM] * 2, (),
    )(t_keep, t_received)
    if t_blocks == 1:
        t_parts = [t_parts[0][b * t_own : (b + 1) * t_own] for b in range(z_count)]
    t_parts = to_z(t_parts)

    pieces = z_count if s_blocks > 1 else 1
    cots, *s_parts = call(
        functools.partial(fold_sp_kernel, s_half, sp_count),
        [shape((sp_count * cot_rows, HEAD), BF16)]
        + [shape((2 * s_half // pieces, HEAD), BF16)] * pieces,
        2 * s_half * HEAD * sp_count, 16 * s_half * HEAD, [VMEM] * sp_count, (),
    )(*messages)
    if s_blocks == 1:
        both = s_parts[0].reshape(2, z_count, s_own, HEAD)
        s_parts = [both[:, b].reshape(2 * s_own, HEAD) for b in range(z_count)]
    s_parts = to_z(s_parts)
    far_cots = to_core(cots)

    grad_target, grad_out = call(
        functools.partial(finish_target_kernel, sp_count, z_count),
        [shape((t_own, width), BF16), shape((q_width, width // sp_count), BF16)],
        2 * q_width * width * t_rows, 2 * q_width * width, [VMEM] * (z_count + sp_count + 4),
        [
            pltpu.VMEM((sp_count * t_rows, width // sp_count), BF16),
            pltpu.VMEM((q_width, sp_count * t_rows), BF16),
        ],
    )(*t_parts, target_part, target_gain, *atts, cots, far_cots)
    grad_source = call(
        functools.partial(finish_source_kernel, z_count), shape((s_own, width), BF16),
        4 * s_own * width * HEAD, 4 * width * HEAD, [VMEM] * (z_count + 5), (),
    )(*s_parts, *prepared)
    return (grad_target, grad_source, grad_out)


def solution(mesh):
    in_specs = (
        P("sp", None),
        P("sp", None),
        P("sp", None),
        P(),
        P(),
        P(None, "tp"),
        P(),
        P(),
        P("tp", None),
    )
    out_specs = (P(("sp", "tp"), None), P(("sp", "tp"), None), P("tp", "sp"))

    return jax.shard_map(
        on_device, mesh=mesh, in_specs=in_specs, out_specs=out_specs, check_vma=False
    )
```
